32 devices in a mesh: sp: 4 (over z), tp: 4 (over y, x), dp: 2 (over core).
Axes of the slice: x: 2, y: 2, z: 4, core: 2. Of those that a mesh axis runs over, the one named last changes fastest.
Arguments:
- latents: bfloat16 [1024, 2048], P(('dp', 'sp', 'tp')), parts along dimension 0, may hold values from -6 to 6
- sample_vector: float32 [2, 2048], P('dp'), parts along dimension 0, may hold values from -6 to 6
- context: bfloat16 [512, 2048], P(('dp', 'sp')), parts along dimension 0, may hold values from -6 to 6
- context_vector: float32 [1, 2048], replicated, may hold values from -6 to 6
- norm_gain: float32 [2048], replicated, may hold values from 0.1 to 1.9
- modulator: bfloat16 [2048, 6144], P(None, ('sp', 'tp')), may hold values from -0.25 to 0.25
- query_weight: bfloat16 [2048, 1024], P('sp', 'tp'), may hold values from -0.125 to 0.125
- key_weight: bfloat16 [2048, 1024], P('sp', 'tp'), may hold values from -0.125 to 0.125
- value_weight: bfloat16 [2048, 2048], P('sp', 'tp'), may hold values from -0.125 to 0.125
- decay_down: bfloat16 [2048, 64], replicated, may hold values from -0.125 to 0.125
- decay_up: bfloat16 [2, 32, 1024], P(None, None, 'tp'), may hold values from -1 to 1
- decay_bias: float32 [2, 1024], P(None, 'tp'), as said below
- decay_extra: float32 [2, 1024, 8], P(None, ('dp', 'sp'), 'tp'), parts along dimension 1, may hold values from -2 to 0
- head_gain: float32 [256], replicated, may hold values from 0.1 to 1.9
- out_weight: bfloat16 [2048, 2048], P('tp'), may hold values from -0.125 to 0.125
Outputs:
- updated: bfloat16 [1024, 2048], P(('dp', 'sp', 'tp')), parts along dimension 0
The draws below stay inside these ranges and needn't reach their ends.
There are 2 independent parts, one for each index of `dp`. The reference program is written for one: setup_inputs(seed, part) draws one part's arguments, and reference() takes and returns one part's arrays. A program takes and returns all parts, laid end to end along the dimension named above; an argument that names none is the same for every part. Nothing has to cross between parts.
Inputs may be any that keep to these rules, and one draw needn't show every extreme that they name: `decay_bias`: offsets of the decay gates,.
All inputs are finite; a program needn't handle non-finite values.
Results may differ from the reference program's by a relative error of at most 0.012.
Values may be sent and summed in bfloat16 or wider, within the bound.
A program may use at most 64 MiB of HBM per device.

```python
import jax
import jax.numpy as jnp
from jax import lax

D = 2048
HEADS = 8
DK = 128
DV = 256
RANK = 32
BLOCK = 64
CTX_LIFT = 4
CTX = 256
TOK_DEV = 128
TOKENS = 512
N_TP = 4


def draw_decay_bias(key, part):
    pick_key, slow_key, fast_key = jax.random.split(jax.random.fold_in(key, 11), 3)
    fast_limit = 5
    is_fast = jax.random.randint(pick_key, (2, HEADS, 1), 0, 10) < fast_limit
    slow_level = jnp.log(1.65 * TOKENS / 4.8)
    slow = slow_level + jax.random.uniform(slow_key, (2, HEADS, DK), jnp.float32, -0.5, 0.5)
    fast = jax.random.uniform(fast_key, (2, HEADS, DK), jnp.float32, -0.5, 1.5)
    return jnp.where(is_fast, fast, slow).reshape(2, HEADS * DK).astype(jnp.float32)


def draw_decay_extra(key, part):
    base_key, place_key, size_key = jax.random.split(jax.random.fold_in(key, 23), 3)
    block_count = TOKENS // TOK_DEV
    rates = jnp.exp(jax.random.uniform(base_key, (2, block_count, HEADS), jnp.float32, jnp.log(0.4), jnp.log(2.5)))
    baseline_magnitude = -(0.8 / TOKENS) * jnp.repeat(rates, TOK_DEV, axis=1)
    places = jax.random.randint(place_key, (2, 2, HEADS), 0, TOKENS)
    objective_totals = jnp.log(1.0 - jax.random.uniform(size_key, (2, 2, HEADS), jnp.float32, 0.2, 0.5))
    positions = jnp.arange(TOKENS, dtype=jnp.int32)
    agreement_tally = positions[None, None, :, None] == places[:, :, None, :]
    cluster_batches = jnp.sum(jnp.where(agreement_tally, objective_totals[:, :, None, :], 0.0), axis=1)
    return (baseline_magnitude + cluster_batches).astype(jnp.float32)


def level_of(stream_key, extent, cuts, smallest, top_value):
    def one(dim, shards_of):
        draws = jax.random.uniform(jax.random.fold_in(jax.random.fold_in(stream_key, 6), dim), (shards_of,), jnp.float32, smallest / len(cuts), top_value / len(cuts))
        return jnp.repeat(jnp.exp(draws), extent[dim] // shards_of).reshape((-1,) + (1,) * (len(extent) - dim - 1))

    factor_of = one(*cuts[0])
    for cut in cuts[1:]:
        factor_of = factor_of * one(*cut)
    return factor_of


def centred(key, dims, width, limit, cuts=(), held_as=jnp.bfloat16):
    drawn = jax.random.normal(key, dims, jnp.float32) * width
    if len(cuts) > 0:
        drawn = level_of(key, dims, cuts, -0.22, 0.18) * drawn
    return jnp.clip(drawn, min=-limit, max=limit).astype(held_as)


def setup_inputs(seed: int = 0, part: int = 0) -> dict:
    splits = jax.random.split(jax.random.key(seed), 16)
    part_keys = jax.random.split(jax.random.fold_in(splits[15], part), 16)
    latents = centred(part_keys[0], (TOKENS, D), 1.0, 6.0, ((0, 16),))
    sample_vector = centred(part_keys[1], (1, D), 1.0, 6.0, (), jnp.float32)
    context = centred(part_keys[2], (CTX, D), 1.0, 6.0, ((0, 4),))
    context_vector = centred(splits[3], (1, D), 1.0, 6.0, (), jnp.float32)
    norm_gain = jnp.clip(1.0 + 0.18 * jax.random.normal(splits[4], (D,), jnp.float32), 0.1, 1.9)
    modulator = centred(splits[5], (D, 3 * D), (D // 4) ** -0.5, 0.25, ((1, 16),))
    query_weight = centred(splits[6], (D, HEADS * DK), D ** -0.5, 0.125, ((0, 4), (1, 4)))
    key_weight = centred(splits[7], (D, HEADS * DK), D ** -0.5, 0.125, ((0, 4), (1, 4)))
    value_weight = centred(splits[8], (D, HEADS * DV), D ** -0.5, 0.125, ((0, 4), (1, 4)))
    decay_down = centred(splits[9], (D, 2 * RANK), D ** -0.5, 0.125)
    decay_up = centred(splits[10], (2, RANK, HEADS * DK), RANK ** -0.5, 1.0, ((2, 4),))
    decay_bias = draw_decay_bias(jax.random.fold_in(splits[15], 71), part)
    decay_extra = draw_decay_extra(jax.random.fold_in(jax.random.fold_in(splits[15], part), 71), part)
    head_gain = jnp.clip(1.0 + 0.18 * jax.random.normal(splits[13], (DV,), jnp.float32), 0.1, 1.9)
    out_weight = centred(splits[14], (HEADS * DV, D), (HEADS * DV) ** -0.5, 0.125, ((0, 4),))
    return dict(latents=latents, sample_vector=sample_vector, context=context, context_vector=context_vector, norm_gain=norm_gain, modulator=modulator, query_weight=query_weight, key_weight=key_weight, value_weight=value_weight, decay_down=decay_down, decay_up=decay_up, decay_bias=decay_bias, decay_extra=decay_extra, head_gain=head_gain, out_weight=out_weight)


epsilon = 1e-06
exponential_sharpness = 16.0
precise = lax.Precision.HIGHEST

def rms_rows(values, gains):
    values = values.astype(jnp.float32)
    return values * lax.rsqrt(lax.optimization_barrier(jnp.mean(values * values, axis=-1, keepdims=True)) + epsilon) * gains

def modulated(tokens, gains, modulation, model_width):
    shift_vector = modulation[:model_width]
    scale_vector = modulation[model_width:2 * model_width]
    return (rms_rows(tokens, gains) * (1.0 + scale_vector) + shift_vector).astype(jnp.bfloat16)

def log_decays(low_rank, decay_up, decay_bias):
    fragment_sequence = []
    for direction in range(2):
        low_piece = lax.optimization_barrier(low_rank[:, direction * RANK:(direction + 1) * RANK]).astype(jnp.float32)
        unnormalized_ratings = jnp.dot(low_piece, decay_up[direction].astype(jnp.float32), precision=precise) + decay_bias[direction]
        fragment_sequence.append(jax.nn.log_sigmoid(unnormalized_ratings) / exponential_sharpness)
    return jnp.stack(fragment_sequence)

def sweep(queries, key_rows, value_rows, decays, carried):
    block_count = queries.shape[0] // BLOCK
    lower_mask = jnp.tril(jnp.ones((BLOCK, BLOCK), dtype=bool))

    def to_blocks(values):
        return values.reshape((block_count, BLOCK) + values.shape[1:])

    def advance(carried, inputs):
        query_block, key_block, value_block, decay_block = inputs
        within = jnp.cumsum(decay_block, axis=0)
        block_total = within[-1]
        query_dec = query_block * jnp.exp(within)
        scores = jnp.einsum('chd,shd->hcs', query_dec, key_block * jnp.exp(-within), precision=precise)
        scores = jnp.where(lower_mask[None], scores, 0.0)
        output = jnp.einsum('hcs,she->che', scores, value_block, precision=precise)
        output = output + jnp.einsum('chd,hde->che', query_dec, carried, precision=precise)
        update = jnp.einsum('shd,she->hde', key_block * jnp.exp(block_total - within), value_block, precision=precise)
        return (jnp.exp(block_total)[:, :, None] * carried + update, output)
    carried, outputs = lax.scan(advance, carried, (to_blocks(queries), to_blocks(key_rows), to_blocks(value_rows), to_blocks(decays)))
    return (carried, outputs.reshape(queries.shape[0], queries.shape[1], value_rows.shape[2]))

def reference(latents, sample_vector, context, context_vector, norm_gain, modulator, query_weight, key_weight, value_weight, decay_down, decay_up, decay_bias, decay_extra, head_gain, out_weight):
    model_width = latents.shape[1]
    conditions = jax.nn.silu(jnp.concatenate([sample_vector, context_vector], 0)).astype(jnp.bfloat16)
    modulation = jnp.dot(conditions, modulator, preferred_element_type=jnp.float32)
    hidden = modulated(latents, norm_gain, modulation[0], model_width)
    context_hidden = modulated(context, norm_gain, modulation[1], model_width)

    def project(token_rows, weight):
        return jnp.dot(token_rows, weight, preferred_element_type=jnp.float32).astype(jnp.bfloat16)

    def by_head(values, size):
        return lax.optimization_barrier(values).astype(jnp.float32).reshape(values.shape[0], HEADS, size)
    queries = by_head(project(hidden, query_weight), DK)
    key_rows = by_head(project(hidden, key_weight), DK)
    value_rows = by_head(project(hidden, value_weight), DV)
    context_keys = by_head(project(context_hidden, key_weight), DK)
    context_values = by_head(project(context_hidden, value_weight), DV)
    decays = log_decays(project(hidden, decay_down), decay_up, decay_bias).reshape(2, TOKENS, HEADS, DK) + decay_extra[:, :, :, None]
    context_decays = log_decays(project(context_hidden, decay_down), decay_up, decay_bias).reshape(2, CTX, HEADS, DK)
    zero_state = jnp.zeros((HEADS, DK, DV), jnp.float32)
    start_forward, _ = sweep(context_keys, context_keys, context_values, context_decays[0], zero_state)
    start_backward, _ = sweep(context_keys[::-1], context_keys[::-1], context_values[::-1], context_decays[1][::-1], zero_state)
    _, forward = sweep(queries, key_rows, value_rows, decays[0], CTX_LIFT * start_forward)
    _, backward = sweep(queries[::-1], key_rows[::-1], value_rows[::-1], decays[1][::-1], CTX_LIFT * start_backward)
    mixed = forward + backward[::-1]
    normed = rms_rows(mixed, head_gain).astype(jnp.bfloat16).reshape(TOKENS, HEADS * DV)
    group_width = HEADS * DV // N_TP
    summed = jnp.zeros((TOKENS, model_width), jnp.float32)
    for group_index in range(N_TP):
        lower_edge = group_index * group_width
        partial_value = jnp.dot(normed[:, lower_edge:lower_edge + group_width], out_weight[lower_edge:lower_edge + group_width], preferred_element_type=jnp.float32).astype(jnp.bfloat16)
        summed = summed + lax.optimization_barrier(partial_value).astype(jnp.float32)
    projected = lax.optimization_barrier(summed.astype(jnp.bfloat16)).astype(jnp.float32)
    gate_vector = modulation[0, 2 * model_width:]
    return (latents.astype(jnp.float32) + gate_vector * projected).astype(jnp.bfloat16)
```

```python
import functools

import jax
import jax.numpy as jnp
from jax import lax
from jax.experimental import pallas as pl
from jax.experimental.pallas import tpu as pltpu
from jax.sharding import PartitionSpec as P

DK = 128
BLOCK = 64
CTX_LIFT = 4
EPS = 1e-06
SHARP = 16.0
F32 = jnp.float32
BF16 = jnp.bfloat16
MESH = pl.DeviceIdType.MESH
HIGH = lax.Precision.HIGHEST


def dot(a, b):
    return jnp.dot(a, b, preferred_element_type=F32)


def dot_nt(a, b):
    return lax.dot_general(a, b, (((1,), (1,)), ((), ())), preferred_element_type=F32)


def dot_tn(a, b):
    return lax.dot_general(a, b, (((0,), (0,)), ((), ())), preferred_element_type=F32)


def sums(mask, values):
    return jnp.dot(mask.astype(F32), values, precision=HIGH, preferred_element_type=F32)


def log_sigmoid(x):
    return jnp.minimum(x, 0.0) - jnp.log1p(jnp.exp(-jnp.abs(x)))


def kernel(
    n_sp,
    n_tp,
    latents,
    sample_vector,
    context,
    context_vector,
    norm_gain,
    modulator,
    query_weight,
    key_weight,
    value_weight,
    decay_down,
    decay_up,
    decay_bias,
    decay_extra,
    head_gain,
    out_weight,
    out,
    mod_w,
    mods,
    lat,
    hid,
    wk,
    wv,
    wq,
    wo,
    acc_k,
    acc_v,
    acc_q,
    c_low,
    c_key,
    c_val,
    st_own,
    st_all,
    tot_own,
    tot_all,
    fold,
    normed,
    part,
    rs,
    loc_sem,
    mod_s,
    mod_r,
    lat_s,
    lat_r,
    w_s,
    w_r,
    p_s,
    p_r,
    cx_s,
    cx_r,
    st_s,
    st_r,
    rs_s,
    rs_r,
):
    s = lax.axis_index("sp")
    t = lax.axis_index("tp")
    d = lax.axis_index("dp")
    h = lax.rem(d, 2)
    mate = d + 1 - 2 * h
    n_dev = n_sp * n_tp
    me = s * n_tp + t
    rows, width = latents.shape
    ctx_rows = context.shape[0]
    length = rows * n_tp
    total = length + ctx_rows
    depth = hid.shape[2]
    half = depth // 2
    heads = decay_bias.shape[1] // DK
    dv = head_gain.shape[1]
    rank = decay_up.shape[1]

    def peer(k):
        other = lax.rem(me + k, n_dev)
        return {"sp": other // n_tp, "tp": lax.rem(other, n_tp)}

    weights = ((key_weight, wk), (value_weight, wv), (query_weight, wq))
    local = [pltpu.make_async_copy(modulator, mod_w, loc_sem.at[0])]
    for m, (source, slots) in enumerate(weights):
        for i in range(2):
            local.append(
                pltpu.make_async_copy(
                    source.at[pl.ds(i * half, half)], slots.at[s, i], loc_sem.at[1 + 2 * m + i]
                )
            )
    local.append(pltpu.make_async_copy(out_weight, wo, loc_sem.at[7]))
    for copy in local:
        copy.start()

    barrier = pltpu.get_barrier_semaphore()
    for k in range(1, n_dev):
        pl.semaphore_signal(barrier, inc=1, device_id=peer(k), device_id_type=MESH)
    pl.semaphore_signal(barrier, inc=1, device_id={"dp": mate}, device_id_type=MESH)
    pl.semaphore_wait(barrier, n_dev)

    def ring_copy(m, r, j, first=False):
        source, slots = weights[m]
        origin = s - j if r == 0 else s + j
        target = s + 1 if r == 0 else s - 1
        src = source.at[pl.ds(h * half, half)] if first else slots.at[origin, h]
        return pltpu.make_async_remote_copy(
            src_ref=src,
            dst_ref=slots.at[origin, h],
            send_sem=w_s.at[m, r, j],
            recv_sem=w_r.at[m, r, j],
            device_id={"sp": target},
            device_id_type=MESH,
        )

    def ring_arrival(m, r, j):
        slots = weights[m][1]
        origin = s - j if r == 0 else s + j
        return pltpu.make_async_remote_copy(
            src_ref=slots.at[origin, h],
            dst_ref=slots.at[origin, h],
            send_sem=w_s.at[m, r, j - 1],
            recv_sem=w_r.at[m, r, j - 1],
            device_id={"sp": s},
            device_id_type=MESH,
        )

    def mate_copy(m, r, j, side):
        slots = weights[m][1]
        origin = s - j if r == 0 else s + j
        return pltpu.make_async_remote_copy(
            src_ref=slots.at[origin, side],
            dst_ref=slots.at[origin, side],
            send_sem=p_s.at[m, r, j - 1],
            recv_sem=p_r.at[m, r, j - 1],
            device_id={"dp": mate},
            device_id_type=MESH,
        )

    def exists(r, j):
        return s - j >= 0 if r == 0 else s + j < n_sp

    def onward(r):
        return s + 1 < n_sp if r == 0 else s - 1 >= 0

    def send_own(m):
        for r in range(2):

            @pl.when(onward(r))
            def _():
                ring_copy(m, r, 0, True).start()

    def relay(m, j):
        for r in range(2):

            @pl.when(exists(r, j))
            def _():
                ring_arrival(m, r, j).wait_recv()
                if j < n_sp - 1:

                    @pl.when(onward(r))
                    def _():
                        ring_copy(m, r, j).start()

                mate_copy(m, r, j, h).start()

    def whole(slots, o):
        return slots[o].reshape(depth, slots.shape[3])

    def multiply(m, j, acc, count):
        slots = weights[m][1]
        for r in range(2):

            @pl.when(exists(r, j))
            def _():
                origin = s - j if r == 0 else s + j
                mate_copy(m, r, j, 1 - h).wait_recv()
                acc[...] += dot(hid[origin, 0:count], whole(slots, origin))

    lat_copies = []
    for k in range(1, n_tp):
        lat_copies.append(
            pltpu.make_async_remote_copy(
                src_ref=latents,
                dst_ref=lat.at[t],
                send_sem=lat_s.at[k],
                recv_sem=lat_r.at[k],
                device_id={"tp": lax.rem(t + k, n_tp)},
                device_id_type=MESH,
            )
        )
    send_own(0)
    send_own(1)
    for copy in lat_copies:
        copy.start()

    is_first = lax.broadcasted_iota(jnp.int32, (16, width), 0) == 0
    vectors = jnp.where(is_first, sample_vector[...], context_vector[...])
    conditions = (vectors / (1.0 + jnp.exp(-vectors))).astype(BF16)
    local[0].wait()
    mods[me] = dot(conditions, mod_w[...])[0:8]
    mod_copies = []
    for k in range(1, n_dev):
        copy = pltpu.make_async_remote_copy(
            src_ref=mods.at[me],
            dst_ref=mods.at[me],
            send_sem=mod_s.at[k],
            recv_sem=mod_r.at[k],
            device_id=peer(k),
            device_id_type=MESH,
        )
        copy.start()
        mod_copies.append(copy)

    lat[t] = latents[...]
    for k in range(1, n_tp):
        pltpu.make_async_remote_copy(
            src_ref=latents,
            dst_ref=lat.at[lax.rem(t - k + n_tp, n_tp)],
            send_sem=lat_s.at[k],
            recv_sem=lat_r.at[k],
            device_id={"tp": t},
            device_id_type=MESH,
        ).wait_recv()
    for k in range(1, n_dev):
        other = lax.rem(me - k + n_dev, n_dev)
        pltpu.make_async_remote_copy(
            src_ref=mods.at[me],
            dst_ref=mods.at[other],
            send_sem=mod_s.at[k],
            recv_sem=mod_r.at[k],
            device_id={"tp": t},
            device_id_type=MESH,
        ).wait_recv()
    modulation = jnp.concatenate([mods[i] for i in range(n_dev)], axis=1)
    gate = modulation[0:1, 2 * width :]

    def modulated(x, row):
        x = x.astype(F32)
        x = x * lax.rsqrt(jnp.mean(x * x, axis=-1, keepdims=True) + EPS) * norm_gain[...]
        shift = modulation[row : row + 1, :width]
        scale = modulation[row : row + 1, width : 2 * width]
        return (x * (1.0 + scale) + shift).astype(BF16)

    def put(x, at):
        count = x.shape[0]
        for o in range(n_sp):
            hid[o, at : at + count] = x[:, o * depth : (o + 1) * depth]

    for i in range(n_tp):
        put(modulated(lat[i], 0), i * rows)
    piece = min(32, ctx_rows)
    for i in range(ctx_rows // piece):
        put(modulated(context[i * piece : (i + 1) * piece], 1), length + i * piece)

    low = dot(hid[0], decay_down[0:depth])
    for o in range(1, n_sp):
        low = low + dot(hid[o], decay_down[o * depth : (o + 1) * depth])
    low = low.astype(BF16)

    def ctx_copy(i, buffer, k):
        other = lax.rem(s + k, n_sp)
        return pltpu.make_async_remote_copy(
            src_ref=buffer.at[s],
            dst_ref=buffer.at[s],
            send_sem=cx_s.at[i, k],
            recv_sem=cx_r.at[i, k],
            device_id={"sp": other},
            device_id_type=MESH,
        )

    def ctx_arrival(i, buffer, k):
        other = lax.rem(s - k + n_sp, n_sp)
        return pltpu.make_async_remote_copy(
            src_ref=buffer.at[s],
            dst_ref=buffer.at[other],
            send_sem=cx_s.at[i, k],
            recv_sem=cx_r.at[i, k],
            device_id={"sp": s},
            device_id_type=MESH,
        )

    c_low[s] = low[length:]
    for k in range(1, n_sp):
        ctx_copy(0, c_low, k).start()

    def log_decays(values, z):
        x = dot(values[:, z * rank : (z + 1) * rank], decay_up[z]) + decay_bias[z : z + 1]
        return log_sigmoid(x) / SHARP

    def wide(z):
        extra = decay_extra[z]
        return jnp.concatenate(
            [jnp.broadcast_to(extra[:, g : g + 1], (length, DK)) for g in range(heads)], axis=1
        )

    row_id = lax.broadcasted_iota(jnp.int32, (length, length), 0)
    col_id = lax.broadcasted_iota(jnp.int32, (length, length), 1)
    same = row_id // BLOCK == col_id // BLOCK
    within = [
        sums(same & (col_id <= row_id), log_decays(low[:length], 0) + wide(0)),
        sums(same & (col_id >= row_id), log_decays(low[:length], 1) + wide(1)),
    ]
    blocks = length // BLOCK
    totals = [
        [within[0][(b + 1) * BLOCK - 1 : (b + 1) * BLOCK] for b in range(blocks)],
        [within[1][b * BLOCK : b * BLOCK + 1] for b in range(blocks)],
    ]
    none = jnp.zeros_like(totals[0][0])

    def between(z, lo, hi):
        value = none
        for b in range(lo, hi):
            value = value + totals[z][b]
        return value

    tot_own[...] = jnp.concatenate(
        [between(0, 0, blocks), between(1, 0, blocks)] + [none] * 6, axis=0
    )

    for k in range(1, n_sp):
        ctx_arrival(0, c_low, k).wait_recv()
    lows = jnp.concatenate([c_low[o] for o in range(n_sp)], axis=0)
    ctx_all = n_sp * ctx_rows
    crow = lax.broadcasted_iota(jnp.int32, (ctx_all, ctx_all), 0)
    ccol = lax.broadcasted_iota(jnp.int32, (ctx_all, ctx_all), 1)
    ctx_weight = [
        jnp.exp(sums(ccol > crow, log_decays(lows, 0))),
        jnp.exp(sums(ccol < crow, log_decays(lows, 1))),
    ]

    for copy in local[1:5]:
        copy.wait()
    acc_k[...] = dot(hid[s], whole(wk, s))
    acc_v[...] = dot(hid[s], whole(wv, s))
    for j in range(1, n_sp):
        relay(0, j)
        relay(1, j)
        if j == n_sp - 1:
            send_own(2)
        multiply(0, j, acc_k, total)
        multiply(1, j, acc_v, total)
    keys = acc_k[...].astype(BF16)
    values = acc_v[...].astype(BF16)
    c_key[s] = keys[length:]
    c_val[s] = values[length:]
    for k in range(1, n_sp):
        ctx_copy(1, c_key, k).start()
        ctx_copy(2, c_val, k).start()
    keys = keys[:length].astype(F32)
    values = values[:length]

    def per_block(f):
        return jnp.concatenate([f(b) for b in range(blocks)], axis=0)

    def rows_of(x, b):
        return x[b * BLOCK : (b + 1) * BLOCK]

    ending = [
        jnp.exp(
            per_block(
                lambda b: totals[0][b] - rows_of(within[0], b) + between(0, b + 1, blocks)
            )
        ),
        jnp.exp(per_block(lambda b: totals[1][b] - rows_of(within[1], b) + between(1, 0, b))),
    ]
    for z in range(2):
        ended = (keys * ending[z]).astype(BF16)
        for g in range(heads):
            st_own[z, g] = dot_tn(
                values[:, g * dv : (g + 1) * dv], ended[:, g * DK : (g + 1) * DK]
            ).astype(BF16)

    def total_copy(z, k):
        to = s + k if z == 0 else s - k
        return pltpu.make_async_remote_copy(
            src_ref=tot_own,
            dst_ref=tot_all.at[z, k],
            send_sem=st_s.at[1, z, k],
            recv_sem=st_r.at[1, z, k],
            device_id={"sp": to},
            device_id_type=MESH,
        )

    def state_pair(z, k):
        to = s + k if z == 0 else s - k
        a = pltpu.make_async_remote_copy(
            src_ref=st_own.at[z],
            dst_ref=st_all.at[z, k],
            send_sem=st_s.at[0, z, k],
            recv_sem=st_r.at[0, z, k],
            device_id={"sp": to},
            device_id_type=MESH,
        )
        return a, total_copy(z, k)

    for k in range(1, n_sp):
        for z in range(2):

            @pl.when(s + k < n_sp if z == 0 else s - k >= 0)
            def _():
                for copy in state_pair(z, k):
                    copy.start()

    for copy in local[5:7]:
        copy.wait()
    acc_q[...] = dot(hid[s, 0:length], whole(wq, s))
    for j in range(1, n_sp):
        relay(2, j)
        multiply(2, j, acc_q, length)
    queries = acc_q[...].astype(BF16).astype(F32)

    tri_row = lax.broadcasted_iota(jnp.int32, (BLOCK, BLOCK), 0)
    tri_col = lax.broadcasted_iota(jnp.int32, (BLOCK, BLOCK), 1)
    masks = [tri_col <= tri_row, tri_col >= tri_row]
    query_dec = [(queries * jnp.exp(within[z])).astype(BF16) for z in range(2)]
    key_dec = [(keys * jnp.exp(-within[z])).astype(BF16) for z in range(2)]
    near = [
        keys * jnp.exp(per_block(lambda b: totals[z][b] - rows_of(within[z], b)))
        for z in range(2)
    ]
    lifted = [
        (queries * jnp.exp(within[0] + per_block(lambda b: between(0, 0, b) + jnp.zeros((BLOCK, 1), F32)))).astype(BF16),
        (queries * jnp.exp(within[1] + per_block(lambda b: between(1, b + 1, blocks) + jnp.zeros((BLOCK, 1), F32)))).astype(BF16),
    ]
    local_out = []
    for g in range(heads):
        cs = slice(g * DK, (g + 1) * DK)
        score_rows = []
        for i in range(blocks):
            line = []
            for j in range(blocks):
                if i == j:
                    score = 0.0
                    for z in range(2):
                        inner = dot_nt(
                            rows_of(query_dec[z], i)[:, cs], rows_of(key_dec[z], j)[:, cs]
                        )
                        score = score + jnp.where(masks[z], inner, 0.0)
                else:
                    z = 0 if j < i else 1
                    gap = between(z, min(i, j) + 1, max(i, j))
                    far = (rows_of(near[z], j) * jnp.exp(gap)).astype(BF16)
                    score = dot_nt(rows_of(query_dec[z], i)[:, cs], far[:, cs])
                line.append(score)
            score_rows.append(jnp.concatenate(line, axis=1))
        scores = jnp.concatenate(score_rows, axis=0).astype(BF16)
        local_out.append(dot(scores, values[:, g * dv : (g + 1) * dv]))

    for k in range(1, n_sp):
        ctx_arrival(1, c_key, k).wait_recv()
        ctx_arrival(2, c_val, k).wait_recv()
    ckeys = jnp.concatenate([c_key[o] for o in range(n_sp)], axis=0).astype(F32)
    cvals = jnp.concatenate([c_val[o] for o in range(n_sp)], axis=0)
    for z in range(2):
        ended = (ckeys * ctx_weight[z]).astype(BF16)
        for g in range(heads):
            fold[z, g] = CTX_LIFT * dot_tn(
                cvals[:, g * dv : (g + 1) * dv], ended[:, g * DK : (g + 1) * DK]
            )

    for k in range(n_sp - 1, 0, -1):
        for z in range(2):

            @pl.when(s - k >= 0 if z == 0 else s + k < n_sp)
            def _():
                for copy in state_pair(z, k):
                    copy.wait_recv()
                decay = jnp.exp(tot_all[z, k][z : z + 1])
                for g in range(heads):
                    fold[z, g] = (
                        fold[z, g] * decay[:, g * DK : (g + 1) * DK]
                        + st_all[z, k, g].astype(F32)
                    )

    for g in range(heads):
        mixed = local_out[g]
        for z in range(2):
            mixed = mixed + dot_nt(
                lifted[z][:, g * DK : (g + 1) * DK], fold[z, g].astype(BF16)
            )
        scale = lax.rsqrt(jnp.mean(mixed * mixed, axis=-1, keepdims=True) + EPS)
        normed[:, g * dv : (g + 1) * dv] = (mixed * scale * head_gain[...]).astype(BF16)

    local[7].wait()
    chunks = rs_s.shape[1]
    span = width // chunks
    rs_copies = []
    for c in range(chunks):
        cols = slice(c * span, (c + 1) * span)
        product = dot(normed[...], wo[:, cols]).astype(BF16)
        for i in range(n_tp):
            part[i, :, cols] = product[i * rows : (i + 1) * rows]
        for k in range(1, n_tp):
            to = lax.rem(t + k, n_tp)
            copy = pltpu.make_async_remote_copy(
                src_ref=part.at[to, :, pl.ds(c * span, span)],
                dst_ref=rs.at[k, :, pl.ds(c * span, span)],
                send_sem=rs_s.at[k, c],
                recv_sem=rs_r.at[k, c],
                device_id={"tp": to},
                device_id_type=MESH,
            )
            copy.start()
            rs_copies.append(copy)
    for c in range(chunks):
        cols = slice(c * span, (c + 1) * span)
        summed = part[t, :, cols].astype(F32)
        for k in range(1, n_tp):
            rs_copies[c * (n_tp - 1) + k - 1].wait_recv()
            summed = summed + rs[k, :, cols].astype(F32)
        projected = summed.astype(BF16).astype(F32)
        out[:, cols] = (latents[:, cols].astype(F32) + gate[:, cols] * projected).astype(BF16)

    for copy in rs_copies + lat_copies + mod_copies:
        copy.wait_send()
    for k in range(1, n_sp):
        for i, buffer in enumerate((c_low, c_key, c_val)):
            ctx_copy(i, buffer, k).wait_send()
        for z in range(2):

            @pl.when(s + k < n_sp if z == 0 else s - k >= 0)
            def _():
                for copy in state_pair(z, k):
                    copy.wait_send()

    for m in range(3):
        for r in range(2):

            @pl.when(onward(r))
            def _():
                ring_copy(m, r, 0, True).wait_send()

            for j in range(1, n_sp):

                @pl.when(exists(r, j))
                def _():
                    mate_copy(m, r, j, h).wait_send()
                    if j < n_sp - 1:

                        @pl.when(onward(r))
                        def _():
                            ring_copy(m, r, j).wait_send()


def per_device(n_sp, n_tp, *args):
    (latents, sv, context, cv, gain, modulator, wq, wk, wv, down, up, bias, extra, hg, wo) = args
    rows, width = latents.shape
    ctx_rows = context.shape[0]
    n_dev = n_sp * n_tp
    length = rows * n_tp
    total = length + ctx_rows
    depth = wq.shape[0]
    kw, vw = wk.shape[1], wv.shape[1]
    heads = bias.shape[1] // DK
    dv = hg.shape[0]
    chunks = 4
    vmem = pl.BlockSpec(memory_space=pltpu.VMEM)
    hbm = pl.BlockSpec(memory_space=pl.ANY)
    dma = pltpu.SemaphoreType.DMA
    scratch = [
        pltpu.VMEM(modulator.shape, BF16),
        pltpu.VMEM((n_dev, 8, modulator.shape[1]), F32),
        pltpu.VMEM((n_tp, rows, width), BF16),
        pltpu.VMEM((n_sp, total, depth), BF16),
        pltpu.VMEM((n_sp, 2, depth // 2, kw), BF16),
        pltpu.VMEM((n_sp, 2, depth // 2, vw), BF16),
        pltpu.VMEM((n_sp, 2, depth // 2, kw), BF16),
        pltpu.VMEM(wo.shape, BF16),
        pltpu.VMEM((total, kw), F32),
        pltpu.VMEM((total, vw), F32),
        pltpu.VMEM((length, kw), F32),
        pltpu.VMEM((n_sp, ctx_rows, down.shape[1]), BF16),
        pltpu.VMEM((n_sp, ctx_rows, kw), BF16),
        pltpu.VMEM((n_sp, ctx_rows, vw), BF16),
        pltpu.VMEM((2, heads, dv, DK), BF16),
        pltpu.VMEM((2, n_sp, heads, dv, DK), BF16),
        pltpu.VMEM((8, kw), F32),
        pltpu.VMEM((2, n_sp, 8, kw), F32),
        pltpu.VMEM((2, heads, dv, DK), F32),
        pltpu.VMEM((length, vw), BF16),
        pltpu.VMEM((n_tp, rows, width), BF16),
        pltpu.VMEM((n_tp, rows, width), BF16),
        dma((8,)),
        dma((n_dev,)),
        dma((n_dev,)),
        dma((n_tp,)),
        dma((n_tp,)),
        dma((3, 2, n_sp)),
        dma((3, 2, n_sp)),
        dma((3, 2, n_sp)),
        dma((3, 2, n_sp)),
        dma((3, n_sp)),
        dma((3, n_sp)),
        dma((2, 2, n_sp)),
        dma((2, 2, n_sp)),
        dma((n_tp, chunks)),
        dma((n_tp, chunks)),
    ]
    return pl.pallas_call(
        functools.partial(kernel, n_sp, n_tp),
        out_shape=jax.ShapeDtypeStruct(latents.shape, BF16),
        in_specs=[vmem] * 5 + [hbm] * 4 + [vmem] * 5 + [hbm],
        out_specs=vmem,
        scratch_shapes=scratch,
        compiler_params=pltpu.CompilerParams(
            collective_id=0, has_side_effects=True, vmem_limit_bytes=56 * 1024 * 1024
        ),
    )(
        latents,
        sv,
        context,
        cv,
        gain.reshape(1, -1),
        modulator,
        wq,
        wk,
        wv,
        down,
        up,
        bias,
        extra,
        hg.reshape(1, -1),
        wo,
    )


def solution(mesh):
    placed = (
        P(("dp", "sp", "tp"), None),
        P("dp", None),
        P(("dp", "sp"), None),
        P(),
        P(),
        P(None, ("sp", "tp")),
        P("sp", "tp"),
        P("sp", "tp"),
        P("sp", "tp"),
        P(),
        P(None, None, "tp"),
        P(None, "tp"),
        P(None, ("dp", "sp"), "tp"),
        P(),
        P("tp", None),
    )
    return jax.shard_map(
        functools.partial(per_device, mesh.shape["sp"], mesh.shape["tp"]),
        mesh=mesh,
        in_specs=placed,
        out_specs=P(("dp", "sp", "tp"), None),
        check_vma=False,
    )
```

```python
import functools

import jax
import jax.numpy as jnp
from jax import lax
from jax.experimental import pallas as pl
from jax.experimental.pallas import tpu as pltpu
from jax.sharding import PartitionSpec as P

DK = 128
BLOCK = 64
CTX_LIFT = 4
EPS = 1e-06
SHARP = 16.0
F32 = jnp.float32
BF16 = jnp.bfloat16
MESH = pl.DeviceIdType.MESH
HIGH = lax.Precision.HIGHEST


def dot(a, b):
    return jnp.dot(a, b, preferred_element_type=F32)


def dot_nt(a, b):
    return lax.dot_general(a, b, (((1,), (1,)), ((), ())), preferred_element_type=F32)


def dot_tn(a, b):
    return lax.dot_general(a, b, (((0,), (0,)), ((), ())), preferred_element_type=F32)


def sums(mask, values):
    return jnp.dot(mask.astype(F32), values, precision=HIGH, preferred_element_type=F32)


def log_sigmoid(x):
    return jnp.minimum(x, 0.0) - jnp.log1p(jnp.exp(-jnp.abs(x)))


def kernel(
    n_sp,
    n_tp,
    latents_in,
    sample_vector_in,
    context_in,
    context_vector_in,
    norm_gain_in,
    modulator,
    query_weight,
    key_weight,
    value_weight,
    decay_down_in,
    decay_up_in,
    decay_bias_in,
    decay_extra_in,
    head_gain_in,
    out_weight,
    out,
    latents,
    sample_vector,
    context,
    context_vector,
    norm_gain,
    decay_down,
    decay_up,
    decay_bias,
    decay_extra,
    head_gain,
    mod_w,
    mods,
    lat,
    hid,
    wk,
    wv,
    wq,
    wo,
    acc_k,
    acc_v,
    acc_q,
    cbuf,
    st_own,
    st_in,
    st_out,
    normed,
    part,
    rs,
    loc_sem,
    mod_s,
    mod_r,
    lat_s,
    lat_r,
    w_s,
    w_r,
    p_s,
    p_r,
    cz_s,
    cz_r,
    ct_s,
    ct_r,
    st_s,
    st_r,
    rs_s,
    rs_r,
):
    s = lax.axis_index("sp")
    t = lax.axis_index("tp")
    d = lax.axis_index("dp")
    h = lax.rem(d, 2)
    mate = d + 1 - 2 * h
    n_dev = n_sp * n_tp
    me = s * n_tp + t
    rows, width = latents.shape
    ctx_rows = context.shape[0]
    length = rows * n_tp
    total = hid.shape[1]
    ctx_all = n_sp * ctx_rows
    depth = hid.shape[2]
    half = depth // 2
    heads = decay_bias.shape[1] // DK
    dv = head_gain.shape[1]
    rank = decay_up.shape[1]

    def peer(k):
        other = lax.rem(me + k, n_dev)
        return {"sp": other // n_tp, "tp": lax.rem(other, n_tp)}

    weights = ((key_weight, wk), (value_weight, wv), (query_weight, wq))
    local = [pltpu.make_async_copy(modulator, mod_w, loc_sem.at[0])]
    for m, (source, slots) in enumerate(weights):
        for i in range(2):
            local.append(
                pltpu.make_async_copy(
                    source.at[pl.ds(i * half, half)], slots.at[s, i], loc_sem.at[1 + 2 * m + i]
                )
            )
    local.append(pltpu.make_async_copy(out_weight, wo, loc_sem.at[7]))
    barrier = pltpu.get_barrier_semaphore()
    for k in range(1, n_dev):
        pl.semaphore_signal(barrier, inc=1, device_id=peer(k), device_id_type=MESH)
    pl.semaphore_signal(barrier, inc=1, device_id={"dp": mate}, device_id_type=MESH)
    small = [
        pltpu.make_async_copy(source, target, loc_sem.at[8 + i])
        for i, (source, target) in enumerate(
            (
                (sample_vector_in, sample_vector),
                (context_vector_in, context_vector),
                (latents_in, latents),
                (context_in, context),
                (norm_gain_in, norm_gain),
                (decay_down_in, decay_down),
                (decay_up_in, decay_up),
                (decay_bias_in, decay_bias),
                (decay_extra_in, decay_extra),
                (head_gain_in, head_gain),
            )
        )
    ]
    for copy in small[:4] + local[:1] + small[4:] + local[1:]:
        copy.start()
    small[2].wait()
    small[3].wait()
    pl.semaphore_wait(barrier, n_dev)

    def ring_copy(m, r, j, first=False):
        source, slots = weights[m]
        origin = s - j if r == 0 else s + j
        target = s + 1 if r == 0 else s - 1
        src = source.at[pl.ds(h * half, half)] if first else slots.at[origin, h]
        return pltpu.make_async_remote_copy(
            src_ref=src,
            dst_ref=slots.at[origin, h],
            send_sem=w_s.at[m, r, j],
            recv_sem=w_r.at[m, r, j],
            device_id={"sp": target},
            device_id_type=MESH,
        )

    def ring_arrival(m, r, j):
        slots = weights[m][1]
        origin = s - j if r == 0 else s + j
        return pltpu.make_async_remote_copy(
            src_ref=slots.at[origin, h],
            dst_ref=slots.at[origin, h],
            send_sem=w_s.at[m, r, j - 1],
            recv_sem=w_r.at[m, r, j - 1],
            device_id={"sp": s},
            device_id_type=MESH,
        )

    def mate_copy(m, r, j, side):
        slots = weights[m][1]
        origin = s - j if r == 0 else s + j
        return pltpu.make_async_remote_copy(
            src_ref=slots.at[origin, side],
            dst_ref=slots.at[origin, side],
            send_sem=p_s.at[m, r, j - 1],
            recv_sem=p_r.at[m, r, j - 1],
            device_id={"dp": mate},
            device_id_type=MESH,
        )

    def exists(r, j):
        return s - j >= 0 if r == 0 else s + j < n_sp

    def onward(r):
        return s + 1 < n_sp if r == 0 else s - 1 >= 0

    def send_own(m):
        for r in range(2):

            @pl.when(onward(r))
            def _():
                ring_copy(m, r, 0, True).start()

    def relay(m, j):
        for r in range(2):

            @pl.when(exists(r, j))
            def _():
                ring_arrival(m, r, j).wait_recv()
                if j < n_sp - 1:

                    @pl.when(onward(r))
                    def _():
                        ring_copy(m, r, j).start()

                mate_copy(m, r, j, h).start()

    def whole(slots, o):
        return slots[o].reshape(depth, slots.shape[3])

    def multiply(m, j, acc, count):
        slots = weights[m][1]
        for r in range(2):

            @pl.when(exists(r, j))
            def _():
                origin = s - j if r == 0 else s + j
                mate_copy(m, r, j, 1 - h).wait_recv()
                acc[...] += dot(hid[origin, 0:count], whole(slots, origin))

    lat_copies = []
    for k in range(1, n_tp):
        lat_copies.append(
            pltpu.make_async_remote_copy(
                src_ref=latents,
                dst_ref=lat.at[t],
                send_sem=lat_s.at[k],
                recv_sem=lat_r.at[k],
                device_id={"tp": lax.rem(t + k, n_tp)},
                device_id_type=MESH,
            )
        )
    span_t = width // n_tp

    def ctx_line(k):
        return pltpu.make_async_remote_copy(
            src_ref=context.at[:, pl.ds(t * span_t, span_t)],
            dst_ref=cbuf.at[s, :, pl.ds(t * span_t, span_t)],
            send_sem=cz_s.at[k],
            recv_sem=cz_r.at[k],
            device_id={"sp": lax.rem(s + k, n_sp)},
            device_id_type=MESH,
        )

    def ctx_line_arrival(k):
        return pltpu.make_async_remote_copy(
            src_ref=context.at[:, pl.ds(t * span_t, span_t)],
            dst_ref=cbuf.at[lax.rem(s - k + n_sp, n_sp), :, pl.ds(t * span_t, span_t)],
            send_sem=cz_s.at[k],
            recv_sem=cz_r.at[k],
            device_id={"sp": s},
            device_id_type=MESH,
        )

    def ctx_plane(k, u, owner):
        view = cbuf.at[lax.rem(s - k + n_sp, n_sp), :, pl.ds(owner * span_t, span_t)]
        return pltpu.make_async_remote_copy(
            src_ref=view,
            dst_ref=view,
            send_sem=ct_s.at[k, u],
            recv_sem=ct_r.at[k, u],
            device_id={"tp": lax.rem(t + u, n_tp)},
            device_id_type=MESH,
        )

    for k in range(1, n_sp):
        ctx_line(k).start()
    for copy in lat_copies:
        copy.start()
    send_own(0)
    send_own(1)
    queue = [(m, j) for j in range(1, n_sp) for m in range(2)]

    def relay_next():
        if queue:
            m, j = queue.pop(0)
            relay(m, j)
            if (m, j) == (1, max(n_sp - 2, 1)):
                send_own(2)

    small[0].wait()
    small[1].wait()
    is_first = lax.broadcasted_iota(jnp.int32, (16, width), 0) == 0
    vectors = jnp.where(is_first, sample_vector[...], context_vector[...])
    conditions = (vectors / (1.0 + jnp.exp(-vectors))).astype(BF16)
    local[0].wait()
    mods[me] = dot(conditions, mod_w[...])[0:2]
    mod_copies = []
    for k in range(1, n_dev):
        copy = pltpu.make_async_remote_copy(
            src_ref=mods.at[me],
            dst_ref=mods.at[me],
            send_sem=mod_s.at[k],
            recv_sem=mod_r.at[k],
            device_id=peer(k),
            device_id_type=MESH,
        )
        copy.start()
        mod_copies.append(copy)

    for k in range(1, n_sp):
        ctx_line_arrival(k).wait_recv()
        for u in range(1, n_tp):
            ctx_plane(k, u, t).start()
    relay_next()
    lat[t] = latents[...]
    cbuf[s] = context[...]
    for k in range(1, n_tp):
        pltpu.make_async_remote_copy(
            src_ref=latents,
            dst_ref=lat.at[lax.rem(t - k + n_tp, n_tp)],
            send_sem=lat_s.at[k],
            recv_sem=lat_r.at[k],
            device_id={"tp": t},
            device_id_type=MESH,
        ).wait_recv()
    for k in range(1, n_dev):
        other = lax.rem(me - k + n_dev, n_dev)
        pltpu.make_async_remote_copy(
            src_ref=mods.at[me],
            dst_ref=mods.at[other],
            send_sem=mod_s.at[k],
            recv_sem=mod_r.at[k],
            device_id={"tp": t},
            device_id_type=MESH,
        ).wait_recv()
    for copy in small[4:]:
        copy.wait()
    modulation = jnp.concatenate([mods[i] for i in range(n_dev)], axis=1)
    gate = modulation[0:1, 2 * width :]

    def modulated(x, row):
        x = x.astype(F32)
        x = x * lax.rsqrt(jnp.mean(x * x, axis=-1, keepdims=True) + EPS) * norm_gain[...]
        shift = modulation[row : row + 1, :width]
        scale = modulation[row : row + 1, width : 2 * width]
        return (x * (1.0 + scale) + shift).astype(BF16)

    def put(x, at):
        count = x.shape[0]
        for o in range(n_sp):
            hid[o, at : at + count] = x[:, o * depth : (o + 1) * depth]

    for i in range(n_tp):
        put(modulated(lat[i], 0), i * rows)
    relay_next()
    for k in range(1, n_sp):
        for u in range(1, n_tp):
            ctx_plane(k, u, lax.rem(t - u + n_tp, n_tp)).wait_recv()
    piece = min(32, ctx_rows)
    for o in range(n_sp):
        for i in range(ctx_rows // piece):
            put(
                modulated(cbuf[o, i * piece : (i + 1) * piece], 1),
                length + o * ctx_rows + i * piece,
            )

    low = dot_nt(hid[0], decay_down[:, 0:depth])
    for o in range(1, n_sp):
        low = low + dot_nt(hid[o], decay_down[:, o * depth : (o + 1) * depth])
    low = low.astype(BF16)

    relay_next()

    def log_decays(values, z):
        x = dot(values[:, z * rank : (z + 1) * rank], decay_up[z]) + decay_bias[z : z + 1]
        return log_sigmoid(x) / SHARP

    row_id = lax.broadcasted_iota(jnp.int32, (length, length), 0)
    col_id = lax.broadcasted_iota(jnp.int32, (length, length), 1)
    same = row_id // BLOCK == col_id // BLOCK
    inner = [same & (col_id <= row_id), same & (col_id >= row_id)]

    def extra_sums(z):
        columns = [
            jnp.sum(jnp.where(inner[z], decay_extra[z, g : g + 1, :], 0.0), axis=1, keepdims=True)
            for g in range(heads)
        ]
        return jnp.concatenate([jnp.broadcast_to(c, (length, DK)) for c in columns], axis=1)

    within = [sums(inner[z], log_decays(low[:length], z)) + extra_sums(z) for z in range(2)]
    blocks = length // BLOCK
    totals = [
        [within[0][(b + 1) * BLOCK - 1 : (b + 1) * BLOCK] for b in range(blocks)],
        [within[1][b * BLOCK : b * BLOCK + 1] for b in range(blocks)],
    ]
    none = jnp.zeros_like(totals[0][0])

    def between(z, lo, hi):
        value = none
        for b in range(lo, hi):
            value = value + totals[z][b]
        return value

    lows = low[length:]
    crow = lax.broadcasted_iota(jnp.int32, (ctx_all, ctx_all), 0)
    ccol = lax.broadcasted_iota(jnp.int32, (ctx_all, ctx_all), 1)
    ctx_weight = [
        jnp.exp(sums(ccol > crow, log_decays(lows, 0))),
        jnp.exp(sums(ccol < crow, log_decays(lows, 1))),
    ]

    for copy in local[1:5]:
        copy.wait()
    acc_k[...] = dot(hid[s], whole(wk, s))
    acc_v[...] = dot(hid[s], whole(wv, s))
    multiply(0, 1, acc_k, total)
    relay_next()
    multiply(1, 1, acc_v, total)
    for j in range(2, n_sp):
        relay_next()
        multiply(0, j, acc_k, total)
        relay_next()
        multiply(1, j, acc_v, total)
    keys = acc_k[...].astype(BF16)
    values = acc_v[...].astype(BF16)
    ckeys = keys[length:].astype(F32)
    cvals = values[length:]
    keys = keys[:length].astype(F32)
    values = values[:length]

    def per_block(f):
        return jnp.concatenate([f(b) for b in range(blocks)], axis=0)

    def rows_of(x, b):
        return x[b * BLOCK : (b + 1) * BLOCK]

    ending = [
        jnp.exp(
            per_block(
                lambda b: totals[0][b] - rows_of(within[0], b) + between(0, b + 1, blocks)
            )
        ),
        jnp.exp(per_block(lambda b: totals[1][b] - rows_of(within[1], b) + between(1, 0, b))),
    ]
    for z in range(2):
        ended = (keys * ending[z]).astype(BF16)
        for g in range(heads):
            st_own[z, g] = dot_tn(
                values[:, g * dv : (g + 1) * dv], ended[:, g * DK : (g + 1) * DK]
            )

    def begins(z):
        return s == 0 if z == 0 else s == n_sp - 1

    def goes_on(z):
        return s < n_sp - 1 if z == 0 else s > 0

    def state_copy(z, g):
        return pltpu.make_async_remote_copy(
            src_ref=st_out.at[z, g],
            dst_ref=st_in.at[z, g],
            send_sem=st_s.at[z, g],
            recv_sem=st_r.at[z, g],
            device_id={"sp": s + 1 if z == 0 else s - 1},
            device_id_type=MESH,
        )

    whole_decay = [jnp.exp(between(z, 0, blocks)) for z in range(2)]

    def pass_on(z, g):
        @pl.when(goes_on(z))
        def _():
            decay = whole_decay[z][:, g * DK : (g + 1) * DK]
            st_out[z, g] = (st_in[z, g].astype(F32) * decay + st_own[z, g]).astype(BF16)
            state_copy(z, g).start()

    for z in range(2):

        @pl.when(begins(z))
        def _():
            ended = (ckeys * ctx_weight[z]).astype(BF16)
            for g in range(heads):
                st_in[z, g] = (
                    CTX_LIFT
                    * dot_tn(cvals[:, g * dv : (g + 1) * dv], ended[:, g * DK : (g + 1) * DK])
                ).astype(BF16)
                pass_on(z, g)

    def chain(near):
        for z in range(2):
            ahead = 2 * s < n_sp - 1 if z == 0 else 2 * s >= n_sp - 1
            turn = ahead if near else jnp.logical_not(ahead)

            @pl.when(jnp.logical_and(turn, jnp.logical_not(begins(z))))
            def _():
                for g in range(heads):
                    state_copy(z, g).wait_recv()
                    pass_on(z, g)

    for copy in local[5:7]:
        copy.wait()
    acc_q[...] = dot(hid[s, 0:length], whole(wq, s))
    for j in range(1, n_sp):
        relay(2, j)
        if j == 1:
            chain(True)
        multiply(2, j, acc_q, length)
        if j == max(n_sp - 2, 1):
            chain(False)
    queries = acc_q[...].astype(BF16).astype(F32)

    tri_row = lax.broadcasted_iota(jnp.int32, (BLOCK, BLOCK), 0)
    tri_col = lax.broadcasted_iota(jnp.int32, (BLOCK, BLOCK), 1)
    masks = [tri_col <= tri_row, tri_col >= tri_row]
    query_dec = [(queries * jnp.exp(within[z])).astype(BF16) for z in range(2)]
    key_dec = [(keys * jnp.exp(-within[z])).astype(BF16) for z in range(2)]
    near = [
        keys * jnp.exp(per_block(lambda b: totals[z][b] - rows_of(within[z], b)))
        for z in range(2)
    ]
    lifted = [
        (queries * jnp.exp(within[0] + per_block(lambda b: between(0, 0, b) + jnp.zeros((BLOCK, 1), F32)))).astype(BF16),
        (queries * jnp.exp(within[1] + per_block(lambda b: between(1, b + 1, blocks) + jnp.zeros((BLOCK, 1), F32)))).astype(BF16),
    ]
    local_out = []
    for g in range(heads):
        cs = slice(g * DK, (g + 1) * DK)
        score_rows = []
        for i in range(blocks):
            line = []
            for j in range(blocks):
                if i == j:
                    score = 0.0
                    for z in range(2):
                        inner = dot_nt(
                            rows_of(query_dec[z], i)[:, cs], rows_of(key_dec[z], j)[:, cs]
                        )
                        score = score + jnp.where(masks[z], inner, 0.0)
                else:
                    z = 0 if j < i else 1
                    gap = between(z, min(i, j) + 1, max(i, j))
                    far = (rows_of(near[z], j) * jnp.exp(gap)).astype(BF16)
                    score = dot_nt(rows_of(query_dec[z], i)[:, cs], far[:, cs])
                line.append(score)
            score_rows.append(jnp.concatenate(line, axis=1))
        scores = jnp.concatenate(score_rows, axis=0).astype(BF16)
        local_out.append(dot(scores, values[:, g * dv : (g + 1) * dv]))

    for g in range(heads):
        mixed = local_out[g]
        for z in range(2):
            mixed = mixed + dot_nt(
                lifted[z][:, g * DK : (g + 1) * DK], st_in[z, g]
            )
        scale = lax.rsqrt(jnp.mean(mixed * mixed, axis=-1, keepdims=True) + EPS)
        normed[:, g * dv : (g + 1) * dv] = (mixed * scale * head_gain[...]).astype(BF16)

    local[7].wait()
    chunks = rs_s.shape[1]
    span = width // chunks
    rs_copies = []
    for c in range(chunks):
        cols = slice(c * span, (c + 1) * span)
        product = dot(normed[...], wo[:, cols]).astype(BF16)
        for i in range(n_tp):
            part[i, :, cols] = product[i * rows : (i + 1) * rows]
        for k in range(1, n_tp):
            to = lax.rem(t + k, n_tp)
            copy = pltpu.make_async_remote_copy(
                src_ref=part.at[to, :, pl.ds(c * span, span)],
                dst_ref=rs.at[k, :, pl.ds(c * span, span)],
                send_sem=rs_s.at[k, c],
                recv_sem=rs_r.at[k, c],
                device_id={"tp": to},
                device_id_type=MESH,
            )
            copy.start()
            rs_copies.append(copy)
    for c in range(chunks):
        cols = slice(c * span, (c + 1) * span)
        summed = part[t, :, cols].astype(F32)
        for k in range(1, n_tp):
            rs_copies[c * (n_tp - 1) + k - 1].wait_recv()
            summed = summed + rs[k, :, cols].astype(F32)
        projected = summed.astype(BF16).astype(F32)
        out[:, cols] = (latents[:, cols].astype(F32) + gate[:, cols] * projected).astype(BF16)

    for copy in rs_copies + lat_copies + mod_copies:
        copy.wait_send()
    for k in range(1, n_sp):
        ctx_line(k).wait_send()
        for u in range(1, n_tp):
            ctx_plane(k, u, t).wait_send()
    for z in range(2):

        @pl.when(goes_on(z))
        def _():
            for g in range(heads):
                state_copy(z, g).wait_send()

    for m in range(3):
        for r in range(2):

            @pl.when(onward(r))
            def _():
                ring_copy(m, r, 0, True).wait_send()

            for j in range(1, n_sp):

                @pl.when(exists(r, j))
                def _():
                    mate_copy(m, r, j, h).wait_send()
                    if j < n_sp - 1:

                        @pl.when(onward(r))
                        def _():
                            ring_copy(m, r, j).wait_send()


def per_device(n_sp, n_tp, *args):
    (latents, sv, context, cv, gain, modulator, wq, wk, wv, down, up, bias, extra, hg, wo) = args
    rows, width = latents.shape
    ctx_rows = context.shape[0]
    n_dev = n_sp * n_tp
    length = rows * n_tp
    total = length + n_sp * ctx_rows
    depth = wq.shape[0]
    kw, vw = wk.shape[1], wv.shape[1]
    heads = bias.shape[1] // DK
    dv = hg.shape[0]
    chunks = 4
    vmem = pl.BlockSpec(memory_space=pltpu.VMEM)
    hbm = pl.BlockSpec(memory_space=pl.ANY)
    dma = pltpu.SemaphoreType.DMA
    scratch = [
        pltpu.VMEM(latents.shape, BF16),
        pltpu.VMEM(sv.shape, F32),
        pltpu.VMEM(context.shape, BF16),
        pltpu.VMEM(cv.shape, F32),
        pltpu.VMEM((1, width), F32),
        pltpu.VMEM(down.shape[::-1], BF16),
        pltpu.VMEM(up.shape, BF16),
        pltpu.VMEM(bias.shape, F32),
        pltpu.VMEM((2, heads, length), F32),
        pltpu.VMEM((1, dv), F32),
        pltpu.VMEM(modulator.shape, BF16),
        pltpu.VMEM((n_dev, 2, modulator.shape[1]), F32),
        pltpu.VMEM((n_tp, rows, width), BF16),
        pltpu.VMEM((n_sp, total, depth), BF16),
        pltpu.VMEM((n_sp, 2, depth // 2, kw), BF16),
        pltpu.VMEM((n_sp, 2, depth // 2, vw), BF16),
        pltpu.VMEM((n_sp, 2, depth // 2, kw), BF16),
        pltpu.VMEM(wo.shape, BF16),
        pltpu.VMEM((total, kw), F32),
        pltpu.VMEM((total, vw), F32),
        pltpu.VMEM((length, kw), F32),
        pltpu.VMEM((n_sp, ctx_rows, width), BF16),
        pltpu.VMEM((2, heads, dv, DK), F32),
        pltpu.VMEM((2, heads, dv, DK), BF16),
        pltpu.VMEM((2, heads, dv, DK), BF16),
        pltpu.VMEM((length, vw), BF16),
        pltpu.VMEM((n_tp, rows, width), BF16),
        pltpu.VMEM((n_tp, rows, width), BF16),
        dma((18,)),
        dma((n_dev,)),
        dma((n_dev,)),
        dma((n_tp,)),
        dma((n_tp,)),
        dma((3, 2, n_sp)),
        dma((3, 2, n_sp)),
        dma((3, 2, n_sp)),
        dma((3, 2, n_sp)),
        dma((n_sp,)),
        dma((n_sp,)),
        dma((n_sp, n_tp)),
        dma((n_sp, n_tp)),
        dma((2, heads)),
        dma((2, heads)),
        dma((n_tp, chunks)),
        dma((n_tp, chunks)),
    ]
    return pl.pallas_call(
        functools.partial(kernel, n_sp, n_tp),
        out_shape=jax.ShapeDtypeStruct(latents.shape, BF16),
        in_specs=[hbm] * 15,
        out_specs=vmem,
        scratch_shapes=scratch,
        compiler_params=pltpu.CompilerParams(
            collective_id=0, has_side_effects=True, vmem_limit_bytes=56 * 1024 * 1024
        ),
    )(
        latents,
        sv,
        context,
        cv,
        gain.reshape(1, -1),
        modulator,
        wq,
        wk,
        wv,
        down.T,
        up,
        bias,
        extra.transpose(0, 2, 1),
        hg.reshape(1, -1),
        wo,
    )


def solution(mesh):
    placed = (
        P(("dp", "sp", "tp"), None),
        P("dp", None),
        P(("dp", "sp"), None),
        P(),
        P(),
        P(None, ("sp", "tp")),
        P("sp", "tp"),
        P("sp", "tp"),
        P("sp", "tp"),
        P(),
        P(None, None, "tp"),
        P(None, "tp"),
        P(None, ("dp", "sp"), "tp"),
        P(),
        P("tp", None),
    )
    return jax.shard_map(
        functools.partial(per_device, mesh.shape["sp"], mesh.shape["tp"]),
        mesh=mesh,
        in_specs=placed,
        out_specs=P(("dp", "sp", "tp"), None),
        check_vma=False,
    )
```
